512 devices in a mesh: kv: 64 (over z, y), tp: 8 (over x, core).
Axes of the slice: x: 4, y: 4, z: 16, core: 2. Of those that a mesh axis runs over, the one named last changes fastest.
Arguments:
- tokens: bfloat16 [32, 4096], P(None, 'kv'), may hold values from -6 to 6
- norm_gain: bfloat16 [4096], P('kv'), may hold values from 0.099609375 to 1.8984375
- w_query: bfloat16 [4096, 4096], P('kv', 'tp'), may hold values from -0.09375 to 0.09375
- w_key: bfloat16 [4096, 1024], P('kv', 'tp'), may hold values from -0.09375 to 0.09375
- w_value: bfloat16 [4096, 1024], P('kv', 'tp'), may hold values from -0.09375 to 0.09375
- w_forget: bfloat16 [4096, 32], P('kv', 'tp'), may hold values from -0.1875 to 0.1875
- forget_bias: float32 [32], P('tp'), may hold values from -1 to 3
- key_cache: bfloat16 [32, 16384, 1024], P(None, 'kv', 'tp'), may hold values from -1200 to 1200
- value_cache: bfloat16 [32, 16384, 1024], P(None, 'kv', 'tp'), may hold values from -6 to 6
- gate_cache: float32 [32, 32, 16384], P(None, 'tp', 'kv'), may hold values from -2051 to 0
- lengths: int32 [32], replicated, may hold values from 4096 to 16383, as said below
- w_out: bfloat16 [4096, 4096], P('tp', 'kv'), may hold values from -0.375 to 0.375
Outputs:
- mixed: bfloat16 [32, 4096], P(None, 'kv')
The draws below stay inside these ranges and needn't reach their ends.
Inputs may be any that keep to these rules, and one draw needn't show every extreme that they name: `lengths`: at least one sequence has the length 16383 in every draw.
All inputs are finite; a program needn't handle non-finite values.
Results may differ from the reference program's by a relative error of at most 0.018.
Values may be sent and summed in bfloat16 or wider, within the bound.
A program may use at most 64 MiB of HBM per device.

```python
import math
import jax
import jax.numpy as jnp
from jax import lax

D = 4096
QUERY_HEADS = 32
KV_HEADS = 8
HEAD_DIM = 128
BATCH_ROWS = 32
P_DEV = 256
CACHE_POSITIONS = 16384
HEADS_DEV = 4
N_TP = 8


def lengths_core(key):
    inner = jax.random.fold_in(key, 11)
    first, second = jax.random.split(inner)
    drawn = jax.random.randint(first, (BATCH_ROWS,), CACHE_POSITIONS // 4, CACHE_POSITIONS)
    longest = jax.random.randint(second, (), 0, BATCH_ROWS)
    drawn = jnp.where(jnp.arange(BATCH_ROWS) == longest, CACHE_POSITIONS - 1, drawn)
    return drawn.astype(jnp.int32)


def draw_lengths(key, part):
    return lengths_core(key)


def draw_gate_cache(key, part):
    seq_len = lengths_core(key)
    key_rows = jax.random.split(jax.random.fold_in(key, 23), 5)
    fast_share = 0.5
    fast = jax.random.uniform(key_rows[0], (QUERY_HEADS,)) < fast_share
    rates = jnp.where(fast, 1.0 / 40.0, 1.0 / CACHE_POSITIONS).astype(jnp.float32)
    block_rates = jnp.exp(jax.random.uniform(key_rows[1], (BATCH_ROWS, 1, CACHE_POSITIONS // P_DEV), jnp.float32, -math.log(2.0), math.log(2.0)))
    block_rates = jnp.repeat(block_rates, P_DEV, axis=2)
    rough = jnp.exp(jax.random.uniform(key_rows[2], (BATCH_ROWS, QUERY_HEADS, CACHE_POSITIONS), jnp.float32, -math.log(2.0), math.log(2.0)))
    gate_logarithms = -rates[None, :, None] * block_rates * rough
    segment_start = jax.random.randint(key_rows[3], (BATCH_ROWS, 3), 0, CACHE_POSITIONS)
    segment_length = jnp.log(jax.random.uniform(key_rows[4], (BATCH_ROWS, 3), jnp.float32, 0.5, 0.8))
    write_position = jnp.arange(CACHE_POSITIONS)
    position_indicator = (write_position[None, None, :] == segment_start[:, :, None]).astype(jnp.float32)
    segment_count = jnp.sum(position_indicator * segment_length[:, :, None], axis=1)
    gate_logarithms = gate_logarithms + segment_count[:, None, :]
    inside = write_position[None, :] < seq_len[:, None]
    gate_logarithms = jnp.where(inside[:, None, :], gate_logarithms, 0.0)
    suffix = jnp.cumsum(gate_logarithms[..., ::-1], axis=-1)[..., ::-1] - gate_logarithms
    return suffix.astype(jnp.float32)


def draw_key_cache(key, part):
    key_rows = jax.random.split(jax.random.fold_in(key, 37), 1)
    base = jnp.clip(jax.random.normal(key_rows[0], (BATCH_ROWS, CACHE_POSITIONS, KV_HEADS * HEAD_DIM), jnp.float32), -6.0, 6.0)
    return base.astype(jnp.bfloat16)


def steps_of(own_key, shape, pieces, low, top_value):
    loudness, own = 1.0, jax.random.fold_in(own_key, 6)
    for dim, blocks in pieces:
        steps = jnp.exp(jax.random.uniform(jax.random.fold_in(own, dim), (blocks,), jnp.float32, low / len(pieces), top_value / len(pieces)))
        loudness = loudness * jnp.repeat(steps, shape[dim] // blocks).reshape([-1 if axis == dim else 1 for axis in range(len(shape))])
    return loudness


def centred(rng, extent, spread, limit, cuts=(), kind=jnp.bfloat16):
    factor_of = steps_of(rng, extent, cuts, -0.22, 0.18) if cuts else 1.0
    values = jax.random.normal(rng, extent, jnp.float32) * spread * factor_of
    return jnp.minimum(jnp.maximum(values, -limit), limit).astype(kind)


def setup_inputs(seed: int = 0) -> dict:
    seeds = jax.random.split(jax.random.key(seed), 13)
    tokens = centred(seeds[0], (BATCH_ROWS, D), 1.0, 6.0, ((1, 64),))
    norm_gain = jnp.clip(1.0 + 0.18 * jax.random.normal(seeds[1], (D,), jnp.float32), 0.099609375, 1.8984375).astype(jnp.bfloat16)
    w_query = centred(seeds[2], (D, QUERY_HEADS * HEAD_DIM), D ** -0.5, 0.09375, ((0, 64), (1, 8)))
    w_key = centred(seeds[3], (D, KV_HEADS * HEAD_DIM), D ** -0.5, 0.09375, ((0, 64), (1, 8)))
    w_value = centred(seeds[4], (D, KV_HEADS * HEAD_DIM), D ** -0.5, 0.09375, ((0, 64), (1, 8)))
    w_forget = centred(seeds[5], (D, QUERY_HEADS), (D // 4) ** -0.5, 0.1875, ((0, 64), (1, 8)))
    forget_bias = jnp.clip(-1.0 + 4.0 * jax.random.uniform(seeds[6], (QUERY_HEADS,), jnp.float32) ** steps_of(seeds[6], (QUERY_HEADS,), ((0, 8),), -0.2, 0.2), -1.0, 3.0)
    key_cache = draw_key_cache(jax.random.fold_in(seeds[12], 71), 0)
    value_cache = centred(seeds[8], (BATCH_ROWS, CACHE_POSITIONS, KV_HEADS * HEAD_DIM), 1.0, 6.0, ((1, 64), (2, 8)))
    gate_cache = draw_gate_cache(jax.random.fold_in(seeds[12], 71), 0)
    lengths = draw_lengths(jax.random.fold_in(seeds[12], 71), 0)
    w_out = centred(seeds[11], (QUERY_HEADS * HEAD_DIM, D), (QUERY_HEADS * HEAD_DIM // 16) ** -0.5, 0.375, ((0, 8), (1, 64)))
    return {"tokens": tokens, "norm_gain": norm_gain, "w_query": w_query, "w_key": w_key, "w_value": w_value, "w_forget": w_forget, "forget_bias": forget_bias, "key_cache": key_cache, "value_cache": value_cache, "gate_cache": gate_cache, "lengths": lengths, "w_out": w_out}


EPSILON = 1e-06
NEGATIVE = -1e+30

def reference(tokens, norm_gain, w_query, w_key, w_value, w_forget, forget_bias, key_cache, value_cache, gate_cache, lengths, w_out):
    batch_rows = tokens.shape[0]
    groups = QUERY_HEADS // KV_HEADS
    score_scaling = HEAD_DIM ** (-0.5)
    tokens_f = tokens.astype(jnp.float32)
    inverse = lax.rsqrt(lax.optimization_barrier(jnp.mean(tokens_f * tokens_f, axis=1)) + EPSILON)
    scaled = (tokens_f * norm_gain.astype(jnp.float32)[None, :]).astype(jnp.bfloat16)
    query_rows = (jnp.dot(scaled, w_query, preferred_element_type=jnp.float32) * inverse[:, None]).astype(jnp.bfloat16)
    fresh_key = (jnp.dot(scaled, w_key, preferred_element_type=jnp.float32) * inverse[:, None]).astype(jnp.bfloat16)
    new_value = (jnp.dot(scaled, w_value, preferred_element_type=jnp.float32) * inverse[:, None]).astype(jnp.bfloat16)
    forget = jnp.dot(scaled, w_forget, preferred_element_type=jnp.float32) * inverse[:, None] + forget_bias[None, :]
    forget_logarithm = jax.nn.log_sigmoid(forget)
    query_float = query_rows.astype(jnp.float32).reshape(batch_rows, KV_HEADS, groups, HEAD_DIM)
    blocks = CACHE_POSITIONS // P_DEV

    def one_block(index):
        start = (index * P_DEV).astype(jnp.int32)
        key_rows = lax.dynamic_slice_in_dim(key_cache, start, P_DEV, 1).astype(jnp.float32).reshape(batch_rows, P_DEV, KV_HEADS, HEAD_DIM)
        values = lax.dynamic_slice_in_dim(value_cache, start, P_DEV, 1).astype(jnp.float32).reshape(batch_rows, P_DEV, KV_HEADS, HEAD_DIM)
        gates = lax.dynamic_slice_in_dim(gate_cache, start, P_DEV, 2)
        scores = jnp.einsum('bkgd,bpkd->bkgp', query_float, key_rows).reshape(batch_rows, QUERY_HEADS, P_DEV)
        scores = scores * score_scaling + gates
        position = start + jnp.arange(P_DEV, dtype=jnp.int32)
        valid = position[None, None, :] < lengths[:, None, None]
        scores = jnp.where(valid, scores, NEGATIVE)
        block_max = lax.optimization_barrier(jnp.max(scores, axis=2))
        weights = jnp.where(valid, jnp.exp(scores - block_max[..., None]), 0.0)
        block_sum = lax.optimization_barrier(jnp.sum(weights, axis=2))
        weights_low = weights.astype(jnp.bfloat16).astype(jnp.float32).reshape(batch_rows, KV_HEADS, groups, P_DEV)
        block_values = jnp.einsum('bkgp,bpkd->bkgd', weights_low, values).reshape(batch_rows, QUERY_HEADS, HEAD_DIM)
        return (block_max, block_sum, block_values)
    block_max, block_sum, block_values = lax.map(one_block, jnp.arange(blocks, dtype=jnp.int32))
    key_float = fresh_key.astype(jnp.float32).reshape(batch_rows, KV_HEADS, HEAD_DIM)
    self_token = jnp.einsum('cptj,cpj->cpt', query_float, key_float).reshape(batch_rows, QUERY_HEADS) * score_scaling - forget_logarithm
    top = jnp.maximum(lax.optimization_barrier(jnp.max(block_max, axis=0)), self_token)
    factor = jnp.exp(block_max - top[None])
    own_weight = jnp.exp(self_token - top)
    total = lax.optimization_barrier(jnp.sum(block_sum * factor, axis=0)) + own_weight
    own_values = jnp.repeat(new_value.astype(jnp.float32).reshape(batch_rows, KV_HEADS, HEAD_DIM), groups, axis=1)
    summed = lax.optimization_barrier(jnp.sum(block_values * factor[..., None], axis=0)) + own_weight[..., None] * own_values
    attended = (summed / total[..., None]).astype(jnp.bfloat16).reshape(batch_rows, N_TP, HEADS_DEV * HEAD_DIM)
    weight_blocks = w_out.astype(jnp.float32).reshape(N_TP, HEADS_DEV * HEAD_DIM, D)
    partial_value = jnp.einsum('bgi,gid->bgd', attended.astype(jnp.float32), weight_blocks)
    partial_value = lax.optimization_barrier(partial_value.astype(jnp.bfloat16)).astype(jnp.float32)
    return lax.optimization_barrier(jnp.sum(partial_value, axis=1)).astype(jnp.bfloat16)
```

```python
import functools

import jax
import jax.numpy as jnp
from jax import lax
from jax.experimental import pallas as pl
from jax.experimental.pallas import tpu as pltpu
from jax.sharding import PartitionSpec as P

HEAD_DIM = 128
ROWS = 8
HEADS = 4
NY = 4
EPSILON = 1e-06
NEGATIVE = -1e30
MESH = pl.DeviceIdType.MESH
NEAR = (-1, 0, 1, 2)


def kernel(
    nz, ny, ntp,
    tokens, gain, w_query, w_key, w_value, w_forget, bias, keys, values, gates, lengths, w_out,
    out,
    tok_v, gain_v, wq_v, wk_v, wv_v, wf_v, wo_v, k_v, v_v, g_v,
    part, ry, acc, sqrow, qz, sqz, kvz, q_all, gp,
    bsend, by, bacc, bstat, bz, bsz, at, ot,
    in_sem, kv_sem, send, recv,
):
    kv, tp = lax.axis_index("kv"), lax.axis_index("tp")
    z, y = kv // ny, lax.rem(kv, ny)
    mine = lax.rem(z, HEADS)
    depth = nz * ny * tokens.shape[1]
    span = keys.shape[1]
    scaling = HEAD_DIM ** (-0.5)

    def at_y(d):
        return (z * ny + lax.rem(y + d, ny), tp)

    def at_z(d):
        return (lax.rem(z + d, nz) * ny + y, tp)

    def at_tp(d):
        return (kv, lax.rem(tp + d, ntp))

    barrier = pltpu.get_barrier_semaphore()
    far_first = sorted(range(1, nz), key=lambda d: -min(d, nz - d))
    for d in far_first:
        pl.semaphore_signal(barrier, inc=1, device_id=at_z(d), device_id_type=MESH)
    for d in range(1, ny):
        pl.semaphore_signal(barrier, inc=1, device_id=at_y(d), device_id_type=MESH)
    for d in range(1, ntp):
        pl.semaphore_signal(barrier, inc=1, device_id=at_tp(d), device_id_type=MESH)

    loads = [
        pltpu.make_async_copy(a, b, in_sem.at[i])
        for i, (a, b) in enumerate(
            (
                (tokens, tok_v), (gain, gain_v), (w_query, wq_v), (w_key, wk_v), (w_value, wv_v),
                (w_forget, wf_v), (gates, g_v),
                (w_out, wo_v.at[0:64]), (w_out, wo_v.at[64:128]),
            )
        )
    ]
    for c in loads:
        c.start()
    k_load = pltpu.make_async_copy(keys, k_v, kv_sem.at[0])
    v_load = pltpu.make_async_copy(values, v_v, kv_sem.at[1])
    k_load.start()
    v_load.start()

    def remote(src, dst, phase, peer):
        return pltpu.make_async_remote_copy(
            src_ref=src, dst_ref=dst, send_sem=send.at[phase], recv_sem=recv.at[phase],
            device_id=peer, device_id_type=MESH,
        )

    def arrived(ref, phase):
        pltpu.make_async_copy(ref, ref, recv.at[phase]).wait()

    def left(ref, phase):
        pltpu.make_async_copy(ref, ref, send.at[phase]).wait()

    lane = lax.broadcasted_iota(jnp.int32, (ROWS, HEAD_DIM), 1)
    row = lax.broadcasted_iota(jnp.int32, (ROWS, HEAD_DIM), 0)
    eye = lane == row

    def as_row(column):
        return jnp.sum(jnp.where(eye, jnp.broadcast_to(column, (ROWS, HEAD_DIM)), 0.0), axis=0, keepdims=True)

    def as_column(line):
        return jnp.sum(jnp.where(eye, jnp.broadcast_to(line, (ROWS, HEAD_DIM)), 0.0), axis=1, keepdims=True)

    for c in loads[:6]:
        c.wait()
    x = tok_v[...].astype(jnp.float32)
    squares = jnp.sum(x * x, axis=1, keepdims=True)
    scaled = (x * gain_v[...].astype(jnp.float32)).astype(jnp.bfloat16)
    for t in range(HEADS):
        p = jnp.dot(scaled, wq_v[:, t * HEAD_DIM : (t + 1) * HEAD_DIM], preferred_element_type=jnp.float32)
        for j in range(ny):
            part[j, t] = p[j * ROWS : (j + 1) * ROWS]
    for t, w in ((4, wk_v), (5, wv_v)):
        p = jnp.dot(scaled, w[...], preferred_element_type=jnp.float32)
        for j in range(ny):
            part[j, t] = p[j * ROWS : (j + 1) * ROWS]
    p = lax.dot_general(scaled, wf_v[...], (((1,), (1,)), ((), ())), preferred_element_type=jnp.float32)
    for j in range(ny):
        side = jnp.broadcast_to(squares[j * ROWS : (j + 1) * ROWS], (ROWS, HEAD_DIM))
        for n in range(HEADS):
            f = jnp.broadcast_to(p[j * ROWS : (j + 1) * ROWS, n : n + 1], (ROWS, HEAD_DIM))
            side = jnp.where(lane == n, f, side)
        part[j, 6] = side

    pl.semaphore_wait(barrier, nz - 1 + ny - 1 + ntp - 1)

    for d in range(1, ny):
        remote(part.at[lax.rem(y + d, ny)], ry.at[d - 1], 0, at_y(d)).start()

    loads[6].wait()
    position = kv * span + lax.broadcasted_iota(jnp.int32, (1, span), 1)
    for j in range(ny):
        for i in range(ROWS):
            b = j * ROWS + i
            valid = position < lengths[b]
            for n in range(HEADS):
                gp[j, n * ROWS + i : n * ROWS + i + 1, :] = jnp.where(valid, g_v[b, n : n + 1, :], NEGATIVE)

    arrived(ry, 0)
    for t in range(7):
        total = part[y, t]
        for d in range(ny - 1):
            total = total + ry[d, t]
        acc[t] = total
    sqrow[...] = as_row(acc[6][:, HEADS : HEADS + 1])

    for d in far_first:
        target = lax.rem(z + d, nz)
        remote(acc.at[lax.rem(target, HEADS)], qz.at[d - 1], 1, at_z(d)).start()
        remote(sqrow, sqz.at[d - 1], 2, at_z(d)).start()

    for d in range(1, nz):
        @pl.when(z == d)
        def _(d=d):
            remote(acc.at[4:7], kvz.at[d - 1], 3, (y, tp)).start()

    arrived(sqz, 2)
    line = sqrow[...]
    for d in range(nz - 1):
        line = line + sqz[d]
    inverse = lax.rsqrt(as_column(line) / depth + EPSILON)
    arrived(qz, 1)
    total = acc[mine]
    for d in range(nz - 1):
        total = total + qz[d]
    slot = y * HEADS + mine
    q_all[slot] = (total * inverse).astype(jnp.bfloat16)

    def spread(ref, slot, phase):
        peers = [(-o, d) for o in NEAR for d in range(ny) if (o, d) != (0, 0)]
        for dz, dy in sorted(peers, key=lambda t: -abs(t[0]) - min(t[1], ny - t[1])):
            peer = (lax.rem(z + dz + nz, nz) * ny + lax.rem(y + dy, ny), tp)
            remote(ref.at[slot], ref.at[slot], phase, peer).start()

    spread(q_all, slot, 4)
    k_load.wait()
    v_load.wait()
    arrived(q_all.at[pl.ds(0, HEADS * ny - 1)], 4)

    tall = lax.rem(lax.broadcasted_iota(jnp.int32, (HEADS * ROWS, 1), 0), ROWS)
    for d in tuple(range(ny // 2, ny)) + tuple(range(1, ny // 2)) + (0,):
        j = lax.rem(y + d, ny)
        q = jnp.concatenate([q_all[j * HEADS + n] for n in range(HEADS)], axis=0)
        scores = jnp.zeros((HEADS * ROWS, span), jnp.float32)
        for i in range(ROWS):
            s = lax.dot_general(q, k_v[j * ROWS + i], (((1,), (1,)), ((), ())), preferred_element_type=jnp.float32)
            scores = jnp.where(tall == i, s, scores)
        scores = scores * scaling + gp[j]
        top = jnp.max(scores, axis=1, keepdims=True)
        weights = jnp.exp(scores - top)
        summed = jnp.sum(weights, axis=1, keepdims=True)
        found = jnp.zeros((HEADS * ROWS, HEAD_DIM), jnp.float32)
        for i in range(ROWS):
            w = jnp.where(tall == i, weights, 0.0).astype(jnp.bfloat16)
            found = found + jnp.dot(w, v_v[j * ROWS + i], preferred_element_type=jnp.float32)
        wide = lax.broadcasted_iota(jnp.int32, (HEADS * ROWS, HEAD_DIM), 1)
        bsend[d, 0] = found
        bsend[d, 1] = jnp.where(wide == 0, top, summed)
        if d:
            remote(bsend.at[d], by.at[d - 1], 5, at_y(d)).start()

    arrived(by, 5)
    tops = [bsend[0, 1][:, 0:1]] + [by[d, 1][:, 0:1] for d in range(ny - 1)]
    top = functools.reduce(jnp.maximum, tops)
    summed = jnp.zeros_like(top)
    found = jnp.zeros((HEADS * ROWS, HEAD_DIM), jnp.float32)
    for k in range(ny):
        block = bsend.at[0] if k == 0 else by.at[k - 1]
        factor = jnp.exp(tops[k] - top)
        summed = summed + block[1][:, 1:2] * factor
        found = found + block[0] * factor
    for n in range(HEADS):
        bacc[n] = found[n * ROWS : (n + 1) * ROWS]
        bstat[n, 0:1] = as_row(top[n * ROWS : (n + 1) * ROWS])
        bstat[n, 1:2] = as_row(summed[n * ROWS : (n + 1) * ROWS])

    @pl.when(z == 0)
    def _():
        arrived(kvz, 3)
        new = [acc[4 + t] for t in range(3)]
        for d in range(nz - 1):
            new = [new[t] + kvz[d, t] for t in range(3)]
        rate = lax.rsqrt(as_column(line) / depth + EPSILON)
        new_key = (new[0] * rate).astype(jnp.bfloat16).astype(jnp.float32)
        new_value = (new[1] * rate).astype(jnp.bfloat16).astype(jnp.float32)
        for n in range(HEADS):
            forget = new[2][:, n : n + 1] * rate + bias[n]
            log_forget = jnp.minimum(forget, 0.0) - jnp.log1p(jnp.exp(-jnp.abs(forget)))
            query = q_all[y * HEADS + n].astype(jnp.float32)
            own = jnp.sum(query * new_key, axis=1, keepdims=True) * scaling - log_forget
            old = top[n * ROWS : (n + 1) * ROWS]
            higher = jnp.maximum(old, own)
            past, now = jnp.exp(old - higher), jnp.exp(own - higher)
            bacc[n] = found[n * ROWS : (n + 1) * ROWS] * past + new_value * now
            bstat[n, 0:1] = as_row(higher)
            bstat[n, 1:2] = as_row(summed[n * ROWS : (n + 1) * ROWS] * past + now)

    for d in far_first:
        target = lax.rem(lax.rem(z + d, nz), HEADS)
        remote(bacc.at[target], bz.at[d - 1], 6, at_z(d)).start()
        remote(bstat.at[target], bsz.at[d - 1], 7, at_z(d)).start()
    arrived(bsz, 7)
    stats = [bstat[mine]] + [bsz[d] for d in range(nz - 1)]
    top = functools.reduce(jnp.maximum, [s[0:1] for s in stats])
    factors = [jnp.exp(s[0:1] - top) for s in stats]
    summed = functools.reduce(jnp.add, [s[1:2] * f for s, f in zip(stats, factors)])
    shares = [as_column(f / summed) for f in factors]
    arrived(bz, 6)
    found = bacc[mine] * shares[0]
    for d in range(nz - 1):
        found = found + bz[d] * shares[d + 1]
    slot = mine * ny + y
    at[slot] = found.astype(jnp.bfloat16)
    spread(at, slot, 8)
    loads[7].wait()
    loads[8].wait()
    arrived(at.at[pl.ds(0, HEADS * ny - 1)], 8)

    total = jnp.zeros((ny * ROWS, 2 * 64), jnp.float32)
    for n in range(HEADS):
        a = jnp.concatenate([at[n * ny + j] for j in range(ny)], axis=0)
        total = total + lax.dot_general(
            a, wo_v[:, n * HEAD_DIM : (n + 1) * HEAD_DIM], (((1,), (1,)), ((), ())), preferred_element_type=jnp.float32
        )
    half = ny * ROWS // 2
    low = lax.broadcasted_iota(jnp.int32, (half, 2 * 64), 1) < 64
    ot[0] = jnp.where(low, total[:half], total[half:]).astype(jnp.bfloat16)
    for d in range(1, ntp):
        remote(ot.at[0], ot.at[d], 9, at_tp(d)).start()
    arrived(ot.at[pl.ds(1, ntp - 1)], 9)
    total = ot[0].astype(jnp.float32)
    for d in range(1, ntp):
        total = total + ot[d].astype(jnp.float32)
    out[0:half] = total[:, 0:64].astype(jnp.bfloat16)
    out[half:] = total[:, 64:].astype(jnp.bfloat16)

    left(ry, 0)
    left(qz, 1)
    left(sqz, 2)
    @pl.when(z != 0)
    def _():
        left(acc.at[4:7], 3)
    left(q_all.at[pl.ds(0, HEADS * ny - 1)], 4)
    left(by, 5)
    left(bz, 6)
    left(bsz, 7)
    left(at.at[pl.ds(0, HEADS * ny - 1)], 8)
    left(ot.at[pl.ds(1, ntp - 1)], 9)


def local(
    nz, ny, ntp,
    tokens, norm_gain, w_query, w_key, w_value, w_forget, forget_bias, key_cache, value_cache, gate_cache, lengths, w_out,
):
    f32, bf16 = jnp.float32, jnp.bfloat16
    rows, span = key_cache.shape[0], key_cache.shape[1]
    wide = HEAD_DIM * HEADS
    args = (
        tokens, norm_gain.reshape(1, -1), w_query, w_key, w_value, w_forget.T, forget_bias,
        key_cache, value_cache, gate_cache, lengths, w_out.T,
    )
    specs = [pl.BlockSpec(memory_space=pl.ANY)] * 12
    specs[6] = specs[10] = pl.BlockSpec(memory_space=pltpu.SMEM)
    own = tokens.shape[1]
    scratch = [
        pltpu.VMEM((rows, own), bf16), pltpu.VMEM((1, own), bf16), pltpu.VMEM((own, wide), bf16),
        pltpu.VMEM((own, HEAD_DIM), bf16), pltpu.VMEM((own, HEAD_DIM), bf16), pltpu.VMEM((HEADS, own), bf16),
        pltpu.VMEM((2 * 64, wide), bf16), pltpu.VMEM((rows, span, HEAD_DIM), bf16), pltpu.VMEM((rows, span, HEAD_DIM), bf16),
        pltpu.VMEM((rows, HEADS, span), f32),
        pltpu.VMEM((ny, 7, ROWS, HEAD_DIM), f32),
        pltpu.VMEM((ny - 1, 7, ROWS, HEAD_DIM), f32),
        pltpu.VMEM((7, ROWS, HEAD_DIM), f32),
        pltpu.VMEM((1, HEAD_DIM), f32),
        pltpu.VMEM((nz - 1, ROWS, HEAD_DIM), f32),
        pltpu.VMEM((nz - 1, 1, HEAD_DIM), f32),
        pltpu.VMEM((nz - 1, 3, ROWS, HEAD_DIM), f32),
        pltpu.VMEM((ny * HEADS, ROWS, HEAD_DIM), bf16),
        pltpu.VMEM((ny, HEADS * ROWS, span), f32),
        pltpu.VMEM((ny, 2, HEADS * ROWS, HEAD_DIM), f32),
        pltpu.VMEM((ny - 1, 2, HEADS * ROWS, HEAD_DIM), f32),
        pltpu.VMEM((HEADS, ROWS, HEAD_DIM), f32),
        pltpu.VMEM((HEADS, 2, HEAD_DIM), f32),
        pltpu.VMEM((nz - 1, ROWS, HEAD_DIM), f32),
        pltpu.VMEM((nz - 1, 2, HEAD_DIM), f32),
        pltpu.VMEM((HEADS * ny, ROWS, HEAD_DIM), bf16),
        pltpu.VMEM((ntp, ny * ROWS // 2, 2 * 64), bf16),
        pltpu.SemaphoreType.DMA((9,)), pltpu.SemaphoreType.DMA((2,)),
        pltpu.SemaphoreType.DMA((10,)), pltpu.SemaphoreType.DMA((10,)),
    ]
    return pl.pallas_call(
        functools.partial(kernel, nz, ny, ntp),
        out_shape=jax.ShapeDtypeStruct((rows, w_out.shape[1]), bf16),
        in_specs=specs,
        out_specs=pl.BlockSpec(memory_space=pltpu.VMEM),
        scratch_shapes=scratch,
        compiler_params=pltpu.CompilerParams(collective_id=0, has_side_effects=True),
        name="step",
    )(*args)


def solution(mesh):
    ny, ntp = NY, mesh.shape["tp"]
    nz = mesh.shape["kv"] // ny
    return jax.shard_map(
        functools.partial(local, nz, ny, ntp),
        mesh=mesh,
        in_specs=(
            P(None, "kv"), P("kv"), P("kv", "tp"), P("kv", "tp"), P("kv", "tp"), P("kv", "tp"), P("tp"),
            P(None, "kv", "tp"), P(None, "kv", "tp"), P(None, "tp", "kv"), P(), P("tp", "kv"),
        ),
        out_specs=P(None, "kv"),
        check_vma=False,
    )
```

```python
import functools

import jax
import jax.numpy as jnp
from jax import lax
from jax.experimental import pallas as pl
from jax.experimental.pallas import tpu as pltpu
from jax.sharding import PartitionSpec as P

HEAD_DIM = 128
ROWS = 8
HEADS = 4
NY = 4
EPSILON = 1e-06
NEGATIVE = -1e30
MESH = pl.DeviceIdType.MESH
NEAR = (-1, 0, 1, 2)


def kernel(
    nz, ny, ntp,
    tokens, gain, w_query, w_key, w_value, w_forget, bias, keys, values, gates, lengths, w_out,
    out,
    tok_v, gain_v, wq_v, wk_v, wv_v, wf_v, wo_v, k_v, v_v, g_v, bias_s, len_s,
    part, ry, acc, sqrow, qz, sqz, kvz, q_all, gp,
    bsend, bstat, by, bys, bz, bsz, own_s, value_s, ots, ot,
    in_sem, send, recv, here,
):
    kv, tp = lax.axis_index("kv"), lax.axis_index("tp")
    z, y = kv // ny, lax.rem(kv, ny)
    mine = lax.rem(z, HEADS)
    depth = nz * ny * tokens.shape[1]
    span = keys.shape[1]
    columns = w_out.shape[0]
    scaling = HEAD_DIM ** (-0.5)

    def turned(i, d, n):
        return jnp.where(i + d < n, i + d, i + d - n)

    def at_y(d):
        return (z * ny + turned(y, d, ny), tp)

    def at_z(d):
        return (turned(z, d, nz) * ny + y, tp)

    loads = [
        pltpu.make_async_copy(a, b, in_sem.at[i])
        for i, (a, b) in enumerate(
            (
                (tokens, tok_v), (gain, gain_v), (w_query, wq_v), (w_key, wk_v), (w_value, wv_v),
                (w_forget, wf_v), (lengths, len_s), (gates, g_v), (bias, bias_s), (keys, k_v), (values, v_v),
                (w_out, wo_v.at[pl.ds(pl.multiple_of(y * columns, columns), columns)]),
            )
        )
    ]
    for c in loads:
        c.start()

    half = nz // 2

    def rank_of(i):
        return i if i < half else nz - 1 + half - i

    rank = jnp.where(z < half, z, nz - 1 + half - z)
    barrier = pltpu.get_barrier_semaphore()
    meetings = (
        [(rank, rank_of(i), (i * ny + y, tp), 0) for i in sorted(range(nz), key=rank_of, reverse=True)]
        + [(y, i, (z * ny + i, tp), 1) for i in range(ny)]
        + [(tp, i, (kv, i), 2) for i in range(ntp)]
    )
    for me, other, peer, _ in meetings:
        @pl.when(me < other)
        def _(peer=peer):
            pl.semaphore_signal(barrier, inc=1, device_id=peer, device_id_type=MESH)
    earlier = rank + y + tp

    @pl.when(earlier > 0)
    def _():
        pl.semaphore_wait(barrier, earlier)

    for kind in range(3):
        pl.semaphore_signal(here.at[kind], inc=1)
    for me, other, peer, kind in meetings:
        @pl.when(me > other)
        def _(peer=peer, kind=kind):
            pl.semaphore_signal(here.at[kind], inc=1, device_id=peer, device_id_type=MESH)

    def remote(src, dst, phase, peer):
        return pltpu.make_async_remote_copy(
            src_ref=src, dst_ref=dst, send_sem=send.at[phase], recv_sem=recv.at[phase],
            device_id=peer, device_id_type=MESH,
        )

    def arrived(ref, phase):
        pltpu.make_async_copy(ref, ref, recv.at[phase]).wait()

    def left(ref, phase):
        pltpu.make_async_copy(ref, ref, send.at[phase]).wait()

    def diagonal(rows):
        shape = (rows, HEAD_DIM)
        return lax.broadcasted_iota(jnp.int32, shape, 1) == lax.broadcasted_iota(jnp.int32, shape, 0)

    def as_row(column):
        return jnp.sum(jnp.where(diagonal(column.shape[0]), column, 0.0), axis=0, keepdims=True)

    def as_column(line, rows):
        return jnp.sum(jnp.where(diagonal(rows), line, 0.0), axis=1, keepdims=True)

    lane = lax.broadcasted_iota(jnp.int32, (ROWS, HEAD_DIM), 1)
    tall_rows = HEADS * ROWS

    for c in loads[:6]:
        c.wait()
    x = tok_v[...].astype(jnp.float32)
    squares = jnp.sum(x * x, axis=1, keepdims=True)
    scaled = (x * gain_v[...].astype(jnp.float32)).astype(jnp.bfloat16)
    for t in range(HEADS):
        p = jnp.dot(scaled, wq_v[:, t * HEAD_DIM : (t + 1) * HEAD_DIM], preferred_element_type=jnp.float32)
        for j in range(ny):
            part[j, t] = p[j * ROWS : (j + 1) * ROWS]
    for t, w in ((4, wk_v), (5, wv_v)):
        p = jnp.dot(scaled, w[...], preferred_element_type=jnp.float32)
        for j in range(ny):
            part[j, t] = p[j * ROWS : (j + 1) * ROWS]
    p = lax.dot_general(scaled, wf_v[...], (((1,), (1,)), ((), ())), preferred_element_type=jnp.float32)
    for j in range(ny):
        side = jnp.broadcast_to(squares[j * ROWS : (j + 1) * ROWS], (ROWS, HEAD_DIM))
        for n in range(HEADS):
            f = jnp.broadcast_to(p[j * ROWS : (j + 1) * ROWS, n : n + 1], (ROWS, HEAD_DIM))
            side = jnp.where(lane == n, f, side)
        part[j, 6] = side

    pl.semaphore_wait(here.at[1], ny - y)
    for d in range(1, ny):
        remote(part.at[turned(y, d, ny)], ry.at[d - 1], 0, at_y(d)).start()

    loads[6].wait()
    loads[7].wait()
    position = kv * span + lax.broadcasted_iota(jnp.int32, (1, span), 1)
    for j in range(ny):
        for i in range(ROWS):
            b = j * ROWS + i
            valid = position < len_s[b]
            for n in range(HEADS):
                gp[j, n * ROWS + i : n * ROWS + i + 1, :] = jnp.where(valid, g_v[b, n : n + 1, :], NEGATIVE)

    arrived(ry, 0)
    for t in range(7):
        total = part[y, t]
        for d in range(ny - 1):
            total = total + ry[d, t]
        acc[t] = total
    sqrow[...] = as_row(acc[6][:, HEADS : HEADS + 1])

    pl.semaphore_wait(here.at[0], nz - rank)
    far_first = sorted(range(1, nz), key=lambda d: -min(d, nz - d))
    for d in far_first:
        remote(acc.at[lax.rem(turned(z, d, nz), HEADS)], qz.at[d - 1], 1, at_z(d)).start()
        remote(sqrow, sqz.at[d - 1], 2, at_z(d)).start()

    for d in range(1, nz):
        @pl.when(z == d)
        def _(d=d):
            remote(acc.at[4:7], kvz.at[d - 1], 3, (y, tp)).start()

    loads[11].wait()
    own_columns = wo_v.at[pl.ds(pl.multiple_of(y * columns, columns), columns)]
    for d in range(1, ny):
        remote(own_columns, own_columns, 4, at_y(d)).start()
    pl.semaphore_wait(here.at[2], ntp - tp)
    for d in range(1, ntp):
        pl.semaphore_signal(here.at[3], inc=1, device_id=(kv, turned(tp, d, ntp)), device_id_type=MESH)

    arrived(sqz, 2)
    line = sqrow[...]
    for d in range(nz - 1):
        line = line + sqz[d]
    rate = lax.rsqrt(as_column(line, ROWS) / depth + EPSILON)
    arrived(qz, 1)
    total = acc[mine]
    for d in range(nz - 1):
        total = total + qz[d]
    slot = y * HEADS + mine
    q_all[slot] = (total * rate).astype(jnp.bfloat16)
    near = [(-o, d) for o in NEAR for d in range(ny) if (o, d) != (0, 0)]
    for dz, dy in sorted(near, key=lambda t: -abs(t[0]) - min(t[1], ny - t[1])):
        peer = (turned(z, dz % nz, nz) * ny + turned(y, dy, ny), tp)
        remote(q_all.at[slot], q_all.at[slot], 5, peer).start()
    loads[9].wait()
    loads[10].wait()
    arrived(q_all.at[pl.ds(0, HEADS * ny - 1)], 5)

    tall = lax.rem(lax.broadcasted_iota(jnp.int32, (tall_rows, 1), 0), ROWS)
    for d in tuple(range(ny // 2, ny)) + tuple(range(1, ny // 2)) + (0,):
        j = turned(y, d, ny)
        q = jnp.concatenate([q_all[j * HEADS + n] for n in range(HEADS)], axis=0)
        scores = jnp.zeros((tall_rows, span), jnp.float32)
        for i in range(ROWS):
            s = lax.dot_general(q, k_v[j * ROWS + i], (((1,), (1,)), ((), ())), preferred_element_type=jnp.float32)
            scores = jnp.where(tall == i, s, scores)
        scores = scores * scaling + gp[j]
        top = jnp.max(scores, axis=1, keepdims=True)
        weights = jnp.exp(scores - top)
        summed = jnp.sum(weights, axis=1, keepdims=True)
        found = jnp.zeros((tall_rows, HEAD_DIM), jnp.float32)
        for i in range(ROWS):
            w = jnp.where(tall == i, weights, 0.0).astype(jnp.bfloat16)
            found = found + jnp.dot(w, v_v[j * ROWS + i], preferred_element_type=jnp.float32)
        top, summed = as_row(top), as_row(summed)
        if d:
            bsend[d - 1] = found.astype(jnp.bfloat16)
            bstat[d - 1, 0:1] = top
            bstat[d - 1, 1:2] = summed
            remote(bsend.at[d - 1], by.at[d - 1], 6, at_y(d)).start()
            remote(bstat.at[d - 1], bys.at[d - 1], 7, at_y(d)).start()

    @pl.when(z == 0)
    def _():
        loads[8].wait()
        arrived(kvz, 3)
        new = [acc[4 + t] for t in range(3)]
        for d in range(nz - 1):
            new = [new[t] + kvz[d, t] for t in range(3)]
        new_key = (new[0] * rate).astype(jnp.bfloat16).astype(jnp.float32)
        value_s[...] = (new[1] * rate).astype(jnp.bfloat16).astype(jnp.float32)
        own = []
        for n in range(HEADS):
            forget = new[2][:, n : n + 1] * rate + bias_s[n]
            log_forget = jnp.minimum(forget, 0.0) - jnp.log1p(jnp.exp(-jnp.abs(forget)))
            query = q_all[y * HEADS + n].astype(jnp.float32)
            own.append(jnp.sum(query * new_key, axis=1, keepdims=True) * scaling - log_forget)
        own_s[...] = as_row(jnp.concatenate(own, axis=0))

    @pl.when(z != 0)
    def _():
        loads[8].wait()

    arrived(bys, 7)
    tops = [top] + [bys[d, 0:1] for d in range(ny - 1)]
    sums = [summed] + [bys[d, 1:2] for d in range(ny - 1)]
    top = functools.reduce(jnp.maximum, tops)
    factors = [jnp.exp(t - top) for t in tops]
    summed = functools.reduce(jnp.add, [s * f for s, f in zip(sums, factors)])
    shares = [as_column(f, tall_rows) for f in factors]
    arrived(by, 6)
    found = found * shares[0]
    for d in range(ny - 1):
        found = found + by[d].astype(jnp.float32) * shares[d + 1]
    last = ny - 1
    bsend[last] = found.astype(jnp.bfloat16)
    bstat[last, 0:1] = top
    bstat[last, 1:2] = summed

    @pl.when(z == 0)
    def _():
        higher = jnp.maximum(top, own_s[...])
        past, now = jnp.exp(top - higher), jnp.exp(own_s[...] - higher)
        value = jnp.concatenate([value_s[...]] * HEADS, axis=0)
        joined = found * as_column(past, tall_rows) + value * as_column(now, tall_rows)
        bsend[last] = joined.astype(jnp.bfloat16)
        bstat[last, 0:1] = higher
        bstat[last, 1:2] = summed * past + now

    for d in far_first:
        remote(bsend.at[last], bz.at[d - 1], 8, at_z(d)).start()
        remote(bstat.at[last], bsz.at[d - 1], 9, at_z(d)).start()
    arrived(wo_v.at[pl.ds(0, (ny - 1) * columns)], 4)
    arrived(bsz, 9)
    stats = [bstat[last]] + [bsz[d] for d in range(nz - 1)]
    top = functools.reduce(jnp.maximum, [s[0:1] for s in stats])
    factors = [jnp.exp(s[0:1] - top) for s in stats]
    summed = functools.reduce(jnp.add, [s[1:2] * f for s, f in zip(stats, factors)])
    shares = [as_column(f / summed, tall_rows) for f in factors]
    arrived(bz, 8)
    found = bsend[last].astype(jnp.float32) * shares[0]
    for d in range(nz - 1):
        found = found + bz[d].astype(jnp.float32) * shares[d + 1]

    found = found.astype(jnp.bfloat16)
    wide = jnp.concatenate([found[n * ROWS : (n + 1) * ROWS] for n in range(HEADS)], axis=1)
    total = lax.dot_general(wide, wo_v[...], (((1,), (1,)), ((), ())), preferred_element_type=jnp.float32)
    pairs = ny // 2
    for k in range(pairs):
        ots[k] = total[:, k * HEAD_DIM : (k + 1) * HEAD_DIM].astype(jnp.bfloat16)

    pl.semaphore_wait(here.at[3], ntp - 1)
    to = [(dy, dt) for dy in range(ny) for dt in range(ntp) if (dy, dt) != (0, 0)]
    for dy, dt in sorted(to, key=lambda t: -min(t[0], ny - t[0]) - min(t[1] // 2, ntp // 2 - t[1] // 2)):
        there = turned(y, dy, ny)
        remote(ots.at[there // 2], ot.at[dt * ny + dy], 10, (z * ny + there, turned(tp, dt, ntp))).start()
    ot[0] = ots[y // 2]
    arrived(ot.at[pl.ds(1, ntp * ny - 1)], 10)
    odd = lax.rem(y, 2) == 1
    for dy in range(ny):
        total = ot[dy].astype(jnp.float32)
        for dt in range(1, ntp):
            total = total + ot[dt * ny + dy].astype(jnp.float32)
        total = jnp.where(odd, pltpu.roll(total, HEAD_DIM // 2, 1), total)
        out[pl.ds(pl.multiple_of(turned(y, ny - dy, ny) * ROWS, ROWS), ROWS)] = total

    left(ry, 0)
    left(qz, 1)
    left(sqz, 2)
    @pl.when(z != 0)
    def _():
        left(acc.at[4:7], 3)
    left(wo_v.at[pl.ds(0, (ny - 1) * columns)], 4)
    left(q_all.at[pl.ds(0, HEADS * ny - 1)], 5)
    left(by, 6)
    left(bys, 7)
    left(bz, 8)
    left(bsz, 9)
    left(ot.at[pl.ds(1, ntp * ny - 1)], 10)


def local(
    nz, ny, ntp,
    tokens, norm_gain, w_query, w_key, w_value, w_forget, forget_bias, key_cache, value_cache, gate_cache, lengths, w_out,
):
    f32, bf16 = jnp.float32, jnp.bfloat16
    rows, span = key_cache.shape[0], key_cache.shape[1]
    wide, columns = HEAD_DIM * HEADS, w_out.shape[1]
    args = (
        tokens, norm_gain.reshape(1, -1), w_query, w_key, w_value, w_forget.T, forget_bias,
        key_cache, value_cache, gate_cache, lengths, w_out.T,
    )
    own = tokens.shape[1]
    scratch = [
        pltpu.VMEM((rows, own), bf16), pltpu.VMEM((1, own), bf16), pltpu.VMEM((own, wide), bf16),
        pltpu.VMEM((own, HEAD_DIM), bf16), pltpu.VMEM((own, HEAD_DIM), bf16), pltpu.VMEM((HEADS, own), bf16),
        pltpu.VMEM((ny * columns, wide), bf16), pltpu.VMEM((rows, span, HEAD_DIM), bf16), pltpu.VMEM((rows, span, HEAD_DIM), bf16),
        pltpu.VMEM((rows, HEADS, span), f32), pltpu.SMEM((HEADS,), f32), pltpu.SMEM((rows,), jnp.int32),
        pltpu.VMEM((ny, 7, ROWS, HEAD_DIM), f32),
        pltpu.VMEM((ny - 1, 7, ROWS, HEAD_DIM), f32),
        pltpu.VMEM((7, ROWS, HEAD_DIM), f32),
        pltpu.VMEM((1, HEAD_DIM), f32),
        pltpu.VMEM((nz - 1, ROWS, HEAD_DIM), f32),
        pltpu.VMEM((nz - 1, 1, HEAD_DIM), f32),
        pltpu.VMEM((nz - 1, 3, ROWS, HEAD_DIM), f32),
        pltpu.VMEM((ny * HEADS, ROWS, HEAD_DIM), bf16),
        pltpu.VMEM((ny, HEADS * ROWS, span), f32),
        pltpu.VMEM((ny, HEADS * ROWS, HEAD_DIM), bf16),
        pltpu.VMEM((ny, 2, HEAD_DIM), f32),
        pltpu.VMEM((ny - 1, HEADS * ROWS, HEAD_DIM), bf16),
        pltpu.VMEM((ny - 1, 2, HEAD_DIM), f32),
        pltpu.VMEM((nz - 1, HEADS * ROWS, HEAD_DIM), bf16),
        pltpu.VMEM((nz - 1, 2, HEAD_DIM), f32),
        pltpu.VMEM((1, HEAD_DIM), f32),
        pltpu.VMEM((ROWS, HEAD_DIM), f32),
        pltpu.VMEM((ny // 2, ROWS, HEAD_DIM), bf16),
        pltpu.VMEM((ntp * ny, ROWS, HEAD_DIM), bf16),
        pltpu.SemaphoreType.DMA((12,)),
        pltpu.SemaphoreType.DMA((11,)), pltpu.SemaphoreType.DMA((11,)), pltpu.SemaphoreType.REGULAR((4,)),
    ]
    mixed = pl.pallas_call(
        functools.partial(kernel, nz, ny, ntp),
        out_shape=pltpu.VMEM((rows, HEAD_DIM), f32),
        in_specs=[pl.BlockSpec(memory_space=pl.ANY)] * 12,
        out_specs=pl.BlockSpec(memory_space=pltpu.VMEM),
        scratch_shapes=scratch,
        compiler_params=pltpu.CompilerParams(collective_id=0, has_side_effects=True),
        name="step",
    )(*args)
    return mixed[:, :columns].astype(bf16)


def solution(mesh):
    ny, ntp = NY, mesh.shape["tp"]
    nz = mesh.shape["kv"] // ny
    return jax.shard_map(
        functools.partial(local, nz, ny, ntp),
        mesh=mesh,
        in_specs=(
            P(None, "kv"), P("kv"), P("kv", "tp"), P("kv", "tp"), P("kv", "tp"), P("kv", "tp"), P("tp"),
            P(None, "kv", "tp"), P(None, "kv", "tp"), P(None, "tp", "kv"), P(), P("tp", "kv"),
        ),
        out_specs=P(None, "kv"),
        check_vma=False,
    )
```

```python
import functools

import jax
import jax.numpy as jnp
from jax import lax
from jax.experimental import pallas as pl
from jax.experimental.pallas import tpu as pltpu
from jax.sharding import PartitionSpec as P

HEAD_DIM = 128
ROWS = 8
HEADS = 4
NY = 4
EPSILON = 1e-06
NEGATIVE = -1e30
MESH = pl.DeviceIdType.MESH
NEAR = (-1, 0, 1, 2)


def kernel(
    nz, ny, ntp,
    tokens, gain, w_query, w_key, w_value, w_forget, bias, keys, values, gates, lengths, w_out,
    out,
    tok_v, gain_v, wq_v, wk_v, wv_v, wf_v, wo_v, k_v, v_v, g_v, bias_s, len_s,
    kt, part, ry, rykv, acc, sqrow, qz, sqz, kvz, q_all, gp,
    bsend, bstat, by, bys, bz, bsz, own_s, value_s, ots, ot,
    in_sem, send, recv, here,
):
    kv, tp = lax.axis_index("kv"), lax.axis_index("tp")
    z, y = kv // ny, lax.rem(kv, ny)
    mine = lax.rem(z, HEADS)
    depth = nz * ny * tokens.shape[1]
    span = keys.shape[1]
    columns = w_out.shape[0]
    scaling = HEAD_DIM ** (-0.5)

    def turned(i, d, n):
        return jnp.where(i + d < n, i + d, i + d - n)

    def at_y(d):
        return (z * ny + turned(y, d, ny), tp)

    def at_z(d):
        return (turned(z, d, nz) * ny + y, tp)

    loads = [
        pltpu.make_async_copy(a, b, in_sem.at[i])
        for i, (a, b) in enumerate(
            (
                (tokens, tok_v), (gain, gain_v), (w_query, wq_v), (w_key, wk_v), (w_value, wv_v),
                (w_forget, wf_v), (lengths, len_s), (gates, g_v), (bias, bias_s), (keys, k_v), (values, v_v),
                (w_out, wo_v.at[pl.ds(pl.multiple_of(y * columns, columns), columns)]),
            )
        )
    ]
    for c in loads:
        c.start()

    barrier = pltpu.get_barrier_semaphore()
    close = sorted({d % nz for d in (2, -2, 1, -1)}, key=lambda d: -min(d, nz - d))
    greeted = [at_z(d) for d in close] + [at_y(d) for d in range(1, ny)]
    for peer in greeted:
        pl.semaphore_signal(barrier, inc=1, device_id=peer, device_id_type=MESH)
    for i in range(ntp):
        @pl.when(tp < i)
        def _(i=i):
            pl.semaphore_signal(barrier, inc=1, device_id=(kv, i), device_id_type=MESH)
    pl.semaphore_wait(barrier, len(greeted) + tp)
    strides = [d for d in (2, 4) if 2 * d <= nz // 2]

    def tell(step):
        for d in (strides[step], nz - strides[step]):
            pl.semaphore_signal(here.at[step], inc=1, device_id=at_z(d), device_id_type=MESH)

    if strides:
        tell(0)
    pl.semaphore_signal(here.at[2], inc=1)
    for i in range(ntp):
        @pl.when(tp > i)
        def _(i=i):
            pl.semaphore_signal(here.at[2], inc=1, device_id=(kv, i), device_id_type=MESH)

    def remote(src, dst, phase, peer):
        return pltpu.make_async_remote_copy(
            src_ref=src, dst_ref=dst, send_sem=send.at[phase], recv_sem=recv.at[phase],
            device_id=peer, device_id_type=MESH,
        )

    def arrived(ref, phase):
        pltpu.make_async_copy(ref, ref, recv.at[phase]).wait()

    def left(ref, phase):
        pltpu.make_async_copy(ref, ref, send.at[phase]).wait()

    def diagonal(rows):
        shape = (rows, HEAD_DIM)
        return lax.broadcasted_iota(jnp.int32, shape, 1) == lax.broadcasted_iota(jnp.int32, shape, 0)

    def as_row(column):
        return jnp.sum(jnp.where(diagonal(column.shape[0]), column, 0.0), axis=0, keepdims=True)

    def as_column(line, rows):
        return jnp.sum(jnp.where(diagonal(rows), line, 0.0), axis=1, keepdims=True)

    lane = lax.broadcasted_iota(jnp.int32, (ROWS, HEAD_DIM), 1)
    tall_rows = HEADS * ROWS

    for c in loads[:6]:
        c.wait()
    x = tok_v[...].astype(jnp.float32)
    squares = jnp.sum(x * x, axis=1, keepdims=True)
    scaled = (x * gain_v[...].astype(jnp.float32)).astype(jnp.bfloat16)
    for t in range(HEADS):
        p = jnp.dot(scaled, wq_v[:, t * HEAD_DIM : (t + 1) * HEAD_DIM], preferred_element_type=jnp.float32)
        for j in range(ny):
            part[j, t] = p[j * ROWS : (j + 1) * ROWS]
    for t, w in ((5, wk_v), (6, wv_v)):
        p = jnp.dot(scaled, w[...], preferred_element_type=jnp.float32)
        for j in range(ny):
            part[j, t] = p[j * ROWS : (j + 1) * ROWS]
    p = lax.dot_general(scaled, wf_v[...], (((1,), (1,)), ((), ())), preferred_element_type=jnp.float32)
    for j in range(ny):
        side = jnp.broadcast_to(squares[j * ROWS : (j + 1) * ROWS], (ROWS, HEAD_DIM))
        for n in range(HEADS):
            f = jnp.broadcast_to(p[j * ROWS : (j + 1) * ROWS, n : n + 1], (ROWS, HEAD_DIM))
            side = jnp.where(lane == n, f, side)
        part[j, 4] = side

    for d in range(1, ny):
        remote(part.at[turned(y, d, ny), 0:5], ry.at[d - 1], 0, at_y(d)).start()
    for d in range(1, ny):
        remote(part.at[turned(y, d, ny), 5:7], rykv.at[d - 1], 11, at_y(d)).start()
    for step in range(1, len(strides)):
        pl.semaphore_wait(here.at[step - 1], 2)
        tell(step)

    loads[6].wait()
    loads[7].wait()
    position = kv * span + lax.broadcasted_iota(jnp.int32, (1, span), 1)
    for j in range(ny):
        for i in range(ROWS):
            b = j * ROWS + i
            valid = position < len_s[b]
            for n in range(HEADS):
                gp[j, n * ROWS + i : n * ROWS + i + 1, :] = jnp.where(valid, g_v[b, n : n + 1, :], NEGATIVE)

    arrived(ry, 0)
    for t in range(5):
        total = part[y, t]
        for d in range(ny - 1):
            total = total + ry[d, t]
        acc[t] = total
    sqrow[...] = as_row(acc[4][:, HEADS : HEADS + 1])

    if strides:
        pl.semaphore_wait(here.at[len(strides) - 1], 2)
    far_first = sorted(range(1, nz), key=lambda d: -min(d, nz - d))
    for d in far_first:
        remote(acc.at[lax.rem(turned(z, d, nz), HEADS)], qz.at[d - 1], 1, at_z(d)).start()
        remote(sqrow, sqz.at[d - 1], 2, at_z(d)).start()

    arrived(rykv, 11)
    for t in range(2):
        total = part[y, 5 + t]
        for d in range(ny - 1):
            total = total + rykv[d, t]
        acc[5 + t] = total
    for d in range(1, nz):
        @pl.when(z == d)
        def _(d=d):
            remote(acc.at[4:7], kvz.at[d - 1], 3, (y, tp)).start()

    loads[11].wait()
    own_columns = wo_v.at[pl.ds(pl.multiple_of(y * columns, columns), columns)]
    for d in range(1, ny):
        remote(own_columns, own_columns, 4, at_y(d)).start()
    pl.semaphore_wait(here.at[2], ntp - tp)
    for d in range(1, ntp):
        pl.semaphore_signal(here.at[3], inc=1, device_id=(kv, turned(tp, d, ntp)), device_id_type=MESH)
    pl.semaphore_signal(here.at[3], inc=1)

    loads[9].wait()

    def turn(b, carry):
        kt[b] = k_v[b].T
        return carry

    lax.fori_loop(0, k_v.shape[0], turn, 0, unroll=4)

    arrived(sqz, 2)
    line = sqrow[...]
    for d in range(nz - 1):
        line = line + sqz[d]
    rate = lax.rsqrt(as_column(line, ROWS) / depth + EPSILON)
    arrived(qz, 1)
    total = acc[mine]
    for d in range(nz - 1):
        total = total + qz[d]
    slot = y * HEADS + mine
    q_all[slot] = (total * rate).astype(jnp.bfloat16)
    near = [(-o, d) for o in NEAR for d in range(ny) if (o, d) != (0, 0)]
    for dz, dy in sorted(near, key=lambda t: -abs(t[0]) - min(t[1], ny - t[1])):
        peer = (turned(z, dz % nz, nz) * ny + turned(y, dy, ny), tp)
        remote(q_all.at[slot], q_all.at[slot], 5, peer).start()
    loads[10].wait()
    arrived(q_all.at[pl.ds(0, HEADS * ny - 1)], 5)

    tall = lax.rem(lax.broadcasted_iota(jnp.int32, (tall_rows, 1), 0), ROWS)
    wanted = sorted(range(1, ny), key=lambda d: -min(d, ny - d))

    def score(d):
        j = turned(y, d, ny)
        q = jnp.concatenate([q_all[j * HEADS + n] for n in range(HEADS)], axis=0)
        scores = jnp.zeros((tall_rows, span), jnp.float32)
        for i in range(ROWS):
            scores = jnp.where(tall == i, jnp.dot(q, kt[j * ROWS + i], preferred_element_type=jnp.float32), scores)
        return scores * scaling + gp[j]

    def weigh(d, scores):
        j = turned(y, d, ny)
        top = jnp.max(scores, axis=1, keepdims=True)
        weights = jnp.exp(scores - top)
        summed = jnp.sum(weights, axis=1, keepdims=True)
        found = jnp.zeros((tall_rows, HEAD_DIM), jnp.float32)
        for i in range(ROWS):
            w = jnp.where(tall == i, weights, 0.0).astype(jnp.bfloat16)
            found = found + jnp.dot(w, v_v[j * ROWS + i], preferred_element_type=jnp.float32)
        return found, as_row(top), as_row(summed)

    def post(d, found, top, summed):
        bsend[d - 1] = found.astype(jnp.bfloat16)
        bstat[d - 1, 0:1] = top
        bstat[d - 1, 1:2] = summed

    def hand(d):
        remote(bsend.at[d - 1], by.at[d - 1], 6, at_y(d)).start()
        remote(bstat.at[d - 1], bys.at[d - 1], 7, at_y(d)).start()

    scores = {d: score(d) for d in wanted}
    for some in (wanted[:1], wanted[1:]):
        for d in some:
            post(d, *weigh(d, scores[d]))
        for d in some:
            hand(d)
    found, top, summed = weigh(0, score(0))

    @pl.when(z == 0)
    def _():
        loads[8].wait()
        arrived(kvz, 3)
        new = [acc[4 + t] for t in range(3)]
        for d in range(nz - 1):
            new = [new[t] + kvz[d, t] for t in range(3)]
        new_key = (new[1] * rate).astype(jnp.bfloat16).astype(jnp.float32)
        value_s[...] = (new[2] * rate).astype(jnp.bfloat16).astype(jnp.float32)
        own = []
        for n in range(HEADS):
            forget = new[0][:, n : n + 1] * rate + bias_s[n]
            log_forget = jnp.minimum(forget, 0.0) - jnp.log1p(jnp.exp(-jnp.abs(forget)))
            query = q_all[y * HEADS + n].astype(jnp.float32)
            own.append(jnp.sum(query * new_key, axis=1, keepdims=True) * scaling - log_forget)
        own_s[...] = as_row(jnp.concatenate(own, axis=0))

    @pl.when(z != 0)
    def _():
        loads[8].wait()

    arrived(bys, 7)
    tops = [top] + [bys[d, 0:1] for d in range(ny - 1)]
    sums = [summed] + [bys[d, 1:2] for d in range(ny - 1)]
    top = functools.reduce(jnp.maximum, tops)
    factors = [jnp.exp(t - top) for t in tops]
    summed = functools.reduce(jnp.add, [s * f for s, f in zip(sums, factors)])
    shares = [as_column(f, tall_rows) for f in factors]
    arrived(by, 6)
    found = found * shares[0]
    for d in range(ny - 1):
        found = found + by[d].astype(jnp.float32) * shares[d + 1]
    last = ny - 1
    bsend[last] = found.astype(jnp.bfloat16)
    bstat[last, 0:1] = top
    bstat[last, 1:2] = summed

    @pl.when(z == 0)
    def _():
        higher = jnp.maximum(top, own_s[...])
        past, now = jnp.exp(top - higher), jnp.exp(own_s[...] - higher)
        value = jnp.concatenate([value_s[...]] * HEADS, axis=0)
        joined = found * as_column(past, tall_rows) + value * as_column(now, tall_rows)
        bsend[last] = joined.astype(jnp.bfloat16)
        bstat[last, 0:1] = higher
        bstat[last, 1:2] = summed * past + now

    for d in far_first:
        remote(bsend.at[last], bz.at[d - 1], 8, at_z(d)).start()
        remote(bstat.at[last], bsz.at[d - 1], 9, at_z(d)).start()
    arrived(wo_v.at[pl.ds(0, (ny - 1) * columns)], 4)
    arrived(bsz, 9)
    stats = [bstat[last]] + [bsz[d] for d in range(nz - 1)]
    top = functools.reduce(jnp.maximum, [s[0:1] for s in stats])
    factors = [jnp.exp(s[0:1] - top) for s in stats]
    summed = functools.reduce(jnp.add, [s[1:2] * f for s, f in zip(stats, factors)])
    shares = [as_column(f / summed, tall_rows) for f in factors]
    arrived(bz, 8)
    found = bsend[last].astype(jnp.float32) * shares[0]
    for d in range(nz - 1):
        found = found + bz[d].astype(jnp.float32) * shares[d + 1]

    found = found.astype(jnp.bfloat16)
    wide = jnp.concatenate([found[n * ROWS : (n + 1) * ROWS] for n in range(HEADS)], axis=1)
    total = lax.dot_general(wide, wo_v[...], (((1,), (1,)), ((), ())), preferred_element_type=jnp.float32)
    pairs = ny // 2
    for k in range(pairs):
        ots[k] = total[:, k * HEAD_DIM : (k + 1) * HEAD_DIM].astype(jnp.bfloat16)

    pl.semaphore_wait(here.at[3], ntp)
    to = [(dy, dt) for dy in range(ny) for dt in range(ntp) if (dy, dt) != (0, 0)]
    for dy, dt in sorted(to, key=lambda t: -min(t[0], ny - t[0]) - min(t[1] // 2, ntp // 2 - t[1] // 2)):
        there = turned(y, dy, ny)
        remote(ots.at[there // 2], ot.at[dt * ny + dy], 10, (z * ny + there, turned(tp, dt, ntp))).start()
    ot[0] = ots[y // 2]
    arrived(ot.at[pl.ds(1, ntp * ny - 1)], 10)
    odd = lax.rem(y, 2) == 1
    for dy in range(ny):
        total = ot[dy].astype(jnp.float32)
        for dt in range(1, ntp):
            total = total + ot[dt * ny + dy].astype(jnp.float32)
        total = jnp.where(odd, pltpu.roll(total, HEAD_DIM // 2, 1), total)
        out[pl.ds(pl.multiple_of(turned(y, ny - dy, ny) * ROWS, ROWS), ROWS)] = total

    left(ry, 0)
    left(rykv, 11)
    left(qz, 1)
    left(sqz, 2)
    @pl.when(z != 0)
    def _():
        left(acc.at[4:7], 3)
    left(wo_v.at[pl.ds(0, (ny - 1) * columns)], 4)
    left(q_all.at[pl.ds(0, HEADS * ny - 1)], 5)
    left(by, 6)
    left(bys, 7)
    left(bz, 8)
    left(bsz, 9)
    left(ot.at[pl.ds(1, ntp * ny - 1)], 10)


def local(
    nz, ny, ntp,
    tokens, norm_gain, w_query, w_key, w_value, w_forget, forget_bias, key_cache, value_cache, gate_cache, lengths, w_out,
):
    f32, bf16 = jnp.float32, jnp.bfloat16
    rows, span = key_cache.shape[0], key_cache.shape[1]
    wide, columns = HEAD_DIM * HEADS, w_out.shape[1]
    args = (
        tokens, norm_gain.reshape(1, -1), w_query, w_key, w_value, w_forget.T, forget_bias,
        key_cache, value_cache, gate_cache, lengths, w_out.T,
    )
    own = tokens.shape[1]
    scratch = [
        pltpu.VMEM((rows, own), bf16), pltpu.VMEM((1, own), bf16), pltpu.VMEM((own, wide), bf16),
        pltpu.VMEM((own, HEAD_DIM), bf16), pltpu.VMEM((own, HEAD_DIM), bf16), pltpu.VMEM((HEADS, own), bf16),
        pltpu.VMEM((ny * columns, wide), bf16), pltpu.VMEM((rows, span, HEAD_DIM), bf16), pltpu.VMEM((rows, span, HEAD_DIM), bf16),
        pltpu.VMEM((rows, HEADS, span), f32), pltpu.SMEM((HEADS,), f32), pltpu.SMEM((rows,), jnp.int32),
        pltpu.VMEM((rows, HEAD_DIM, span), bf16),
        pltpu.VMEM((ny, 7, ROWS, HEAD_DIM), f32),
        pltpu.VMEM((ny - 1, 5, ROWS, HEAD_DIM), f32),
        pltpu.VMEM((ny - 1, 2, ROWS, HEAD_DIM), f32),
        pltpu.VMEM((7, ROWS, HEAD_DIM), f32),
        pltpu.VMEM((1, HEAD_DIM), f32),
        pltpu.VMEM((nz - 1, ROWS, HEAD_DIM), f32),
        pltpu.VMEM((nz - 1, 1, HEAD_DIM), f32),
        pltpu.VMEM((nz - 1, 3, ROWS, HEAD_DIM), f32),
        pltpu.VMEM((ny * HEADS, ROWS, HEAD_DIM), bf16),
        pltpu.VMEM((ny, HEADS * ROWS, span), f32),
        pltpu.VMEM((ny, HEADS * ROWS, HEAD_DIM), bf16),
        pltpu.VMEM((ny, 2, HEAD_DIM), f32),
        pltpu.VMEM((ny - 1, HEADS * ROWS, HEAD_DIM), bf16),
        pltpu.VMEM((ny - 1, 2, HEAD_DIM), f32),
        pltpu.VMEM((nz - 1, HEADS * ROWS, HEAD_DIM), bf16),
        pltpu.VMEM((nz - 1, 2, HEAD_DIM), f32),
        pltpu.VMEM((1, HEAD_DIM), f32),
        pltpu.VMEM((ROWS, HEAD_DIM), f32),
        pltpu.VMEM((ny // 2, ROWS, HEAD_DIM), bf16),
        pltpu.VMEM((ntp * ny, ROWS, HEAD_DIM), bf16),
        pltpu.SemaphoreType.DMA((12,)),
        pltpu.SemaphoreType.DMA((12,)), pltpu.SemaphoreType.DMA((12,)), pltpu.SemaphoreType.REGULAR((4,)),
    ]
    mixed = pl.pallas_call(
        functools.partial(kernel, nz, ny, ntp),
        out_shape=pltpu.VMEM((rows, HEAD_DIM), f32),
        in_specs=[pl.BlockSpec(memory_space=pl.ANY)] * 12,
        out_specs=pl.BlockSpec(memory_space=pltpu.VMEM),
        scratch_shapes=scratch,
        compiler_params=pltpu.CompilerParams(collective_id=0, has_side_effects=True),
        name="step",
    )(*args)
    return mixed[:, :columns].astype(bf16)


def solution(mesh):
    ny, ntp = NY, mesh.shape["tp"]
    nz = mesh.shape["kv"] // ny
    return jax.shard_map(
        functools.partial(local, nz, ny, ntp),
        mesh=mesh,
        in_specs=(
            P(None, "kv"), P("kv"), P("kv", "tp"), P("kv", "tp"), P("kv", "tp"), P("kv", "tp"), P("tp"),
            P(None, "kv", "tp"), P(None, "kv", "tp"), P(None, "tp", "kv"), P(), P("tp", "kv"),
        ),
        out_specs=P(None, "kv"),
        check_vma=False,
    )
```
